32 devices in a mesh: sp: 8 (over z, y), tp: 4 (over x, core).
Axes of the slice: x: 2, y: 2, z: 4, core: 2. Of those that a mesh axis runs over, the one named last changes fastest.
Arguments:
- tokens: bfloat16 [3072, 2048], P('sp', 'tp'), may hold values from -6 to 6
- norm_gain: float32 [2048], replicated, may hold values from 0.1 to 1.9
- w_glu_value: bfloat16 [2048, 2048], P(None, 'tp'), may hold values from -0.125 to 0.125
- w_glu_gate: bfloat16 [2048, 2048], P(None, 'tp'), may hold values from -0.125 to 0.125
- w_query: bfloat16 [2048, 2048], P(None, 'tp'), may hold values from -0.125 to 0.125
- w_key: bfloat16 [2048, 2048], P(None, 'tp'), may hold values from -0.125 to 0.125
- w_value: bfloat16 [2048, 2048], P(None, 'tp'), may hold values from -0.125 to 0.125
- score_offset: float32 [32], P('tp'), may hold values from -15 to -4, as said below
- conv_taps: bfloat16 [31, 2048], P(None, 'tp'), may hold values from -1 to 1
- conv_gain: float32 [2048], replicated, may hold values from 0.1 to 1.9
- w_conv_out: bfloat16 [2048, 2048], P(None, 'tp'), may hold values from -0.125 to 0.125
- w_attn_out: bfloat16 [2048, 2048], P(None, 'tp'), may hold values from -1 to 1
- w_gate_conv: bfloat16 [2048, 2048], P(None, 'tp'), may hold values from -0.125 to 0.125
- w_gate_attn: bfloat16 [2048, 2048], P(None, 'tp'), may hold values from -0.125 to 0.125
Outputs:
- mixed: bfloat16 [3072, 2048], P('sp', 'tp')
- log_weight: float32 [32, 3072], P('tp', 'sp')
The draws below stay inside these ranges and needn't reach their ends.
Inputs may be any that keep to these rules, and one draw needn't show every extreme that they name: `score_offset`: per-head score offsets.
All inputs are finite; a program needn't handle non-finite values.
Results may differ from the reference program's by a relative error of at most 0.0078.
Values may be sent and summed in bfloat16 or wider, within the bound.
A program may use at most 128 MiB of HBM per device.

```python
import jax
import jax.numpy as jnp
from jax import lax

D = 2048
HEADS = 32
HEAD = 64
WIDTH = 31
TOK_DEV = 384
TOKENS = 3072
N_SP = 8


def draw_score_offset(key, part):
    return jax.random.uniform(key, (HEADS,), jnp.float32, -14.0, -4.0)


def shard_levels(stream_key, shape, cuts, low, largest):
    def one(dim, shards_of):
        steps = jax.random.uniform(jax.random.fold_in(jax.random.fold_in(stream_key, 6), dim), (shards_of,), jnp.float32, low / len(cuts), largest / len(cuts))
        return jnp.repeat(jnp.exp(steps), shape[dim] // shards_of).reshape((-1,) + (1,) * (len(shape) - dim - 1))

    loudness = one(*cuts[0])
    for cut in cuts[1:]:
        loudness = loudness * one(*cut)
    return loudness


def centred(own_key, extent, spread, limit, split=(), held_as=jnp.bfloat16):
    factor_of = shard_levels(own_key, extent, split, -0.22, 0.18) if split else 1.0
    entries = jax.random.normal(own_key, extent, jnp.float32) * spread * factor_of
    return jnp.minimum(jnp.maximum(entries, -limit), limit).astype(held_as)


def setup_inputs(seed: int = 0) -> dict:
    streams_of = jax.random.split(jax.random.key(seed), 15)
    tokens = centred(streams_of[0], (TOKENS, D), 1.0, 6.0, ((0, 8), (1, 4)))
    norm_gain = jnp.clip(1.0 + 0.18 * jax.random.normal(streams_of[1], (D,), jnp.float32), 0.1, 1.9)
    w_glu_value = centred(streams_of[2], (D, D), D ** -0.5, 0.125, ((1, 4),))
    w_glu_gate = centred(streams_of[3], (D, D), D ** -0.5, 0.125, ((1, 4),))
    w_query = centred(streams_of[4], (D, D), D ** -0.5, 0.125, ((1, 4),))
    w_key = centred(streams_of[5], (D, D), D ** -0.5, 0.125, ((1, 4),))
    w_value = centred(streams_of[6], (D, D), D ** -0.5, 0.125, ((1, 4),))
    score_offset = draw_score_offset(jax.random.fold_in(streams_of[14], 71), 0)
    conv_taps = centred(streams_of[8], (WIDTH, D), WIDTH ** -0.5, 1.0, ((1, 4),))
    conv_gain = jnp.clip(1.0 + 0.18 * jax.random.normal(streams_of[9], (D,), jnp.float32), 0.1, 1.9)
    w_conv_out = centred(streams_of[10], (D, D), D ** -0.5, 0.125, ((1, 4),))
    w_attn_out = centred(streams_of[11], (D, D), HEADS ** -0.5, 1.0, ((1, 4),))
    w_gate_conv = centred(streams_of[12], (D, D), D ** -0.5, 0.125, ((1, 4),))
    w_gate_attn = centred(streams_of[13], (D, D), D ** -0.5, 0.125, ((1, 4),))
    return {"tokens": tokens, "norm_gain": norm_gain, "w_glu_value": w_glu_value, "w_glu_gate": w_glu_gate, "w_query": w_query, "w_key": w_key, "w_value": w_value, "score_offset": score_offset, "conv_taps": conv_taps, "conv_gain": conv_gain, "w_conv_out": w_conv_out, "w_attn_out": w_attn_out, "w_gate_conv": w_gate_conv, "w_gate_attn": w_gate_attn}


def reference(tokens, norm_gain, w_glu_value, w_glu_gate, w_query, w_key, w_value, score_offset, conv_taps, conv_gain, w_conv_out, w_attn_out, w_gate_conv, w_gate_attn):
    features = tokens.astype(jnp.float32)
    normed = (features * lax.rsqrt(lax.optimization_barrier(jnp.mean(features * features, axis=-1, keepdims=True)) + 1e-06) * norm_gain).astype(jnp.bfloat16)
    glued = (jnp.dot(normed, w_glu_value, preferred_element_type=jnp.float32) * jax.nn.sigmoid(jnp.dot(normed, w_glu_gate, preferred_element_type=jnp.float32))).astype(jnp.bfloat16)
    queries = jnp.dot(normed, w_query, preferred_element_type=jnp.float32).astype(jnp.bfloat16)
    keys = jnp.dot(normed, w_key, preferred_element_type=jnp.float32).astype(jnp.bfloat16)
    values = jnp.dot(normed, w_value, preferred_element_type=jnp.float32).astype(jnp.bfloat16)
    padded = jnp.concatenate([jnp.zeros((WIDTH - 1, D), jnp.bfloat16), glued], axis=0)
    tap_rows = conv_taps.astype(jnp.float32)
    convolved = jnp.zeros((TOKENS, D), jnp.float32)
    for tap in range(WIDTH):
        convolved = convolved + tap_rows[tap] * padded[tap:tap + TOKENS].astype(jnp.float32)
    convolved = convolved.astype(jnp.bfloat16)
    conv_float = convolved.astype(jnp.float32)
    channel_mean = lax.optimization_barrier(jnp.mean(conv_float, axis=-1, keepdims=True))
    channel_var = lax.optimization_barrier(jnp.mean(conv_float * conv_float, axis=-1, keepdims=True)) - channel_mean * channel_mean
    conv_act = jax.nn.silu((conv_float - channel_mean) * lax.rsqrt(channel_var + 1e-05) * conv_gain).astype(jnp.bfloat16)
    score_scale = 1.0 / HEAD ** 0.5
    query_heads = queries.reshape(TOKENS, HEADS, HEAD).transpose(1, 0, 2)
    key_heads = keys.reshape(TOKENS, HEADS, HEAD).transpose(1, 0, 2)
    value_heads = values.reshape(TOKENS, HEADS, HEAD).transpose(1, 0, 2)

    def one_head(packed):
        query_one, key_one, value_one, offset_one = packed

        def one_block(begin_at):
            query_block = lax.dynamic_slice_in_dim(query_one, begin_at, TOK_DEV, 0)
            scores = jnp.dot(query_block, key_one.T, preferred_element_type=jnp.float32) * score_scale + offset_one
            query_pos = begin_at + jnp.arange(TOK_DEV).astype(jnp.int32)
            key_pos = jnp.arange(TOKENS).astype(jnp.int32)
            allowed = key_pos[None, :] <= query_pos[:, None]
            softened = jnp.where(allowed, jax.nn.softplus(scores), 0.0)
            behind = lax.cumsum(softened, axis=1, reverse=True)
            stick = jnp.where(allowed, jnp.exp(scores - behind), 0.0).astype(jnp.bfloat16)
            block_out = jnp.dot(stick, value_one, preferred_element_type=jnp.float32).astype(jnp.bfloat16)
            block_log = jnp.log(-jnp.expm1(-behind[:, 0]))
            return (block_out, block_log)
        starts = (jnp.arange(N_SP) * TOK_DEV).astype(jnp.int32)
        outs, logs = lax.map(one_block, starts)
        return (outs.reshape(TOKENS, HEAD), logs.reshape(TOKENS))
    head_outs, log_weight = lax.map(one_head, (query_heads, key_heads, value_heads, score_offset))
    attended = head_outs.transpose(1, 0, 2).reshape(TOKENS, D)
    gate_conv = jax.nn.sigmoid(jnp.dot(normed, w_gate_conv, preferred_element_type=jnp.float32))
    gate_attn = jax.nn.sigmoid(jnp.dot(normed, w_gate_attn, preferred_element_type=jnp.float32))
    conv_branch = jnp.dot(conv_act, w_conv_out, preferred_element_type=jnp.float32)
    attn_branch = jnp.dot(attended, w_attn_out, preferred_element_type=jnp.float32)
    mixed = (gate_conv * conv_branch + gate_attn * attn_branch).astype(jnp.bfloat16)
    return (mixed, log_weight)
```

```python
import functools

import jax
import jax.numpy as jnp
from jax import lax
from jax.experimental import pallas as pl
from jax.experimental.pallas import tpu as pltpu
from jax.sharding import PartitionSpec as P

HEAD = 64
WIDTH = 31


key_span = 512


def passed_along(array, axis, by):
    length = lax.axis_size(axis)
    pairs = [(i, i + by) for i in range(length) if 0 <= i + by < length]
    return lax.ppermute(array, axis, pairs)


def sweep_block(
    sweep_state, key_block, value_block, key_first, query_first, query_heads, offsets, score_scale
):
    summed, spent_stick = sweep_state
    head_count = offsets.shape[0]
    query_count = query_heads.shape[0]
    key_count = key_block.shape[0]
    key_heads = key_block.reshape(key_count, head_count, -1)
    value_heads = value_block.reshape(key_count, head_count, -1)
    scores = (
        jnp.einsum("thd,shd->hts", query_heads, key_heads, preferred_element_type=jnp.float32)
        * score_scale
        + offsets[:, None, None]
    )
    query_pos = query_first + lax.iota(jnp.int32, query_count)
    key_pos = key_first + lax.iota(jnp.int32, key_count)
    allowed = (key_pos[None, :] <= query_pos[:, None]) & (key_pos[None, :] >= 0)
    softened = jnp.where(allowed[None], jax.nn.softplus(scores), 0.0)
    behind = lax.cumsum(softened, axis=2, reverse=True)
    stick = jnp.where(
        allowed[None], jnp.exp(scores - behind - spent_stick[:, :, None]), 0.0
    ).astype(jnp.bfloat16)
    summed = summed + jnp.einsum(
        "hts,shd->thd", stick, value_heads, preferred_element_type=jnp.float32
    )
    return (summed, spent_stick + behind[:, :, 0])


def softplus_parts(z):
    x = jnp.exp(-jnp.abs(z))
    tail = jnp.where(x < 0.004, x - (0.5 * x) * x, jnp.log(1.0 + x))
    return jnp.maximum(z, 0.0) + tail, jnp.minimum(z, 0.0) - tail


def stick_kernel(
    query_span, strip, cell, width, scale, offset_ref, packed_ref, out_ref, spent_ref,
    query_s, key_s, value_s, acc_s, carry_s
):
    block = pl.program_id(1)

    @pl.when(block == 0)
    def _():
        query_s[...] = packed_ref[0, :, :width]
        key_s[...] = packed_ref[0, :, width : 2 * width]
        value_s[...] = packed_ref[0, :, 2 * width :]

    offset = offset_ref[0, pl.program_id(0)]
    later = (
        lax.broadcasted_iota(jnp.int32, (cell, cell), 0)
        > lax.broadcasted_iota(jnp.int32, (cell, cell), 1)
    ).astype(jnp.bfloat16)
    acc_s[...] = jnp.zeros_like(acc_s)
    carry_s[...] = jnp.zeros_like(carry_s)
    query_first = pl.multiple_of(block * query_span, query_span)

    def one(row, key_first, diagonal):
        rows = pl.ds(row, strip)
        query = query_s[pl.ds(query_first + row, strip), :]
        keys = key_s[pl.ds(key_first, cell), :]
        z = (
            lax.dot_general(
                query, keys, (((1,), (1,)), ((), ())), preferred_element_type=jnp.float32
            )
            * scale
            + offset
        )
        soft, own = softplus_parts(z)
        if diagonal:
            allowed = lax.broadcasted_iota(jnp.int32, z.shape, 1) <= lax.broadcasted_iota(
                jnp.int32, z.shape, 0
            )
            soft = jnp.where(allowed, soft, 0.0)
        behind = jnp.dot(soft.astype(jnp.bfloat16), later, preferred_element_type=jnp.float32)
        carry = carry_s[rows, :]
        stick = jnp.exp(own - behind - carry)
        if diagonal:
            stick = jnp.where(allowed, stick, 0.0)
        acc_s[rows, :] += jnp.dot(
            stick.astype(jnp.bfloat16),
            value_s[pl.ds(key_first, cell), :],
            preferred_element_type=jnp.float32,
        )
        carry_s[rows, :] = carry + jnp.sum(soft, axis=1, keepdims=True)

    for col in range(query_span - cell, -1, -cell):
        for row in range(col, query_span, strip):
            one(row, query_first + col, row == col)

    def turn(index, _):
        first = pl.multiple_of(query_first - (index + 1) * query_span, query_span)
        for col in range(query_span - cell, -1, -cell):
            for row in range(0, query_span, strip):
                one(row, first + col, False)
        return 0

    lax.fori_loop(0, block, turn, 0)
    out_ref[0] = acc_s[...].astype(out_ref.dtype)
    spent_ref[0] = jnp.transpose(jnp.broadcast_to(carry_s[...], (query_span, 128)))[:1]


def stick_attention(packed, offsets, scale):
    heads, positions, wide = packed.shape
    width = wide // 3
    cell = next(c for c in (256, 128, 64, 32, 16, 8, positions) if positions % c == 0)
    query_span = 2 * cell if positions % (2 * cell) == 0 else cell
    out, spent = pl.pallas_call(
        functools.partial(stick_kernel, query_span, cell, cell, width, scale),
        grid=(heads, positions // query_span),
        in_specs=[
            pl.BlockSpec(memory_space=pltpu.SMEM),
            pl.BlockSpec((1, positions, wide), lambda h, b: (h, 0, 0)),
        ],
        out_specs=[
            pl.BlockSpec((1, query_span, width), lambda h, b: (h, b, 0)),
            pl.BlockSpec((1, 1, query_span), lambda h, b: (h, 0, b)),
        ],
        out_shape=[
            jax.ShapeDtypeStruct((heads, positions, width), jnp.bfloat16),
            jax.ShapeDtypeStruct((heads, 1, positions), jnp.float32),
        ],
        scratch_shapes=[
            pltpu.VMEM((positions, width), jnp.bfloat16),
            pltpu.VMEM((positions, width), jnp.bfloat16),
            pltpu.VMEM((positions, width), jnp.bfloat16),
            pltpu.VMEM((query_span, width), jnp.float32),
            pltpu.VMEM((query_span, 1), jnp.float32),
        ],
        compiler_params=pltpu.CompilerParams(
            dimension_semantics=("arbitrary", "arbitrary"), vmem_limit_bytes=32 << 20
        ),
        cost_estimate=pl.CostEstimate(
            flops=6 * heads * positions * positions * width,
            bytes_accessed=8 * heads * positions * width,
            transcendentals=3 * heads * positions * positions // 2,
        ),
    )(offsets, packed)
    return out, spent[:, 0]


def exchanged_attention(queries, keys, values, score_offset, score_scale):
    tok_rows, columns = queries.shape
    length = lax.axis_size("sp")
    head_count = score_offset.shape[0]
    own_heads = head_count // length
    width = columns // head_count
    packed = jnp.stack([queries, keys, values], axis=1)
    packed = packed.reshape(tok_rows, 3, length, own_heads, width).transpose(2, 3, 0, 1, 4)
    packed = packed.reshape(length, own_heads, tok_rows, 3 * width)
    packed = lax.all_to_all(packed, "sp", 0, 0)
    packed = packed.transpose(1, 0, 2, 3).reshape(own_heads, length * tok_rows, 3 * width)
    own = lax.dynamic_slice_in_dim(score_offset, lax.axis_index("sp") * own_heads, own_heads, 0)
    out, spent = stick_attention(packed, own[None], score_scale)
    out = out.reshape(own_heads, length, tok_rows, width).transpose(1, 0, 2, 3)
    spent = spent.reshape(own_heads, length, tok_rows).transpose(1, 0, 2)
    out = lax.all_to_all(out, "sp", 0, 0)
    spent = lax.all_to_all(spent, "sp", 0, 0)
    attended = out.transpose(2, 0, 1, 3).reshape(tok_rows, columns)
    return attended, spent.reshape(head_count, tok_rows)


def gathered_attention(queries, keys, values, score_offset, score_scale):
    tok_rows = queries.shape[0]
    head_count = score_offset.shape[0]
    head_width = queries.shape[1] // head_count
    query_heads = queries.reshape(tok_rows, head_count, head_width)
    own_index = lax.axis_index("sp")
    query_first = own_index * tok_rows
    start_state = (
        jnp.zeros((tok_rows, head_count, head_width), jnp.float32),
        jnp.zeros((head_count, tok_rows), jnp.float32),
    )
    gathered = (
        lax.all_gather(keys, "sp", axis=0, tiled=True),
        lax.all_gather(values, "sp", axis=0, tiled=True),
    )
    leading = jnp.zeros((key_span, keys.shape[1]), jnp.bfloat16)
    all_keys = jnp.concatenate([leading, gathered[0]], axis=0)
    all_values = jnp.concatenate([leading, gathered[1]], axis=0)
    key_end = (own_index + 1) * tok_rows
    turns = (key_end + key_span - 1) // key_span

    def advance(turn_index, sweep_state):
        key_first = key_end - (turn_index + 1) * key_span
        key_block = lax.dynamic_slice_in_dim(all_keys, key_first + key_span, key_span, 0)
        value_block = lax.dynamic_slice_in_dim(all_values, key_first + key_span, key_span, 0)
        return sweep_block(
            sweep_state,
            key_block,
            value_block,
            key_first,
            query_first,
            query_heads,
            score_offset,
            score_scale,
        )

    summed, spent_stick = lax.fori_loop(0, turns, advance, start_state)
    return summed.reshape(tok_rows, head_count * head_width).astype(jnp.bfloat16), spent_stick


def body(
    tokens,
    norm_gain,
    w_glu_value,
    w_glu_gate,
    w_query,
    w_key,
    w_value,
    score_offset,
    conv_taps,
    conv_gain,
    w_conv_out,
    w_attn_out,
    w_gate_conv,
    w_gate_attn,
):
    whole_rows = lax.all_gather(tokens, "tp", axis=1, tiled=True)
    features = whole_rows.astype(jnp.float32)
    normed = (
        features
        * lax.rsqrt(jnp.mean(features * features, axis=-1, keepdims=True) + 1e-06)
        * norm_gain
    ).astype(jnp.bfloat16)
    glued = (
        jnp.dot(normed, w_glu_value, preferred_element_type=jnp.float32)
        * jax.nn.sigmoid(jnp.dot(normed, w_glu_gate, preferred_element_type=jnp.float32))
    ).astype(jnp.bfloat16)
    queries = jnp.dot(normed, w_query, preferred_element_type=jnp.float32).astype(jnp.bfloat16)
    keys = jnp.dot(normed, w_key, preferred_element_type=jnp.float32).astype(jnp.bfloat16)
    values = jnp.dot(normed, w_value, preferred_element_type=jnp.float32).astype(jnp.bfloat16)
    tok_rows = whole_rows.shape[0]
    tap_count = conv_taps.shape[0]
    channels = glued.shape[1]
    previous = passed_along(glued[tok_rows - (tap_count - 1) :], "sp", 1)
    extended = jnp.concatenate([previous, glued], axis=0)
    tap_rows = conv_taps.astype(jnp.float32)
    convolved = jnp.zeros((tok_rows, channels), jnp.float32)
    for tap in range(WIDTH):
        convolved = convolved + tap_rows[tap] * extended[tap : tap + tok_rows].astype(jnp.float32)
    convolved = convolved.astype(jnp.bfloat16)
    head_count = score_offset.shape[0]
    head_width = queries.shape[1] // head_count
    score_scale = 1.0 / head_width**0.5
    attention = (
        exchanged_attention if head_count % lax.axis_size("sp") == 0 else gathered_attention
    )
    attended, spent_stick = attention(queries, keys, values, score_offset, score_scale)
    log_weight = jnp.log(-jnp.expm1(-spent_stick))
    gate_conv = jax.nn.sigmoid(jnp.dot(normed, w_gate_conv, preferred_element_type=jnp.float32))
    gate_attn = jax.nn.sigmoid(jnp.dot(normed, w_gate_attn, preferred_element_type=jnp.float32))
    all_channels = conv_gain.shape[0]
    conv_float = convolved.astype(jnp.float32)
    channel_sum, channel_squares = lax.psum(
        (
            jnp.sum(conv_float, axis=-1, keepdims=True),
            jnp.sum(conv_float * conv_float, axis=-1, keepdims=True),
        ),
        "tp",
    )
    channel_mean = channel_sum / all_channels
    channel_var = channel_squares / all_channels - channel_mean * channel_mean
    local_gain = lax.dynamic_slice_in_dim(conv_gain, lax.axis_index("tp") * channels, channels, 0)
    conv_act = jax.nn.silu(
        (conv_float - channel_mean) * lax.rsqrt(channel_var + 1e-05) * local_gain
    ).astype(jnp.bfloat16)
    conv_piece = lax.all_gather(conv_act, "tp", axis=1, tiled=True)
    attn_piece = lax.all_gather(attended, "tp", axis=1, tiled=True)
    conv_branch = jnp.dot(conv_piece, w_conv_out, preferred_element_type=jnp.float32)
    attn_branch = jnp.dot(attn_piece, w_attn_out, preferred_element_type=jnp.float32)
    mixed = (gate_conv * conv_branch + gate_attn * attn_branch).astype(jnp.bfloat16)
    return (mixed, log_weight)


def solution(mesh):
    in_specs = (
        P("sp", "tp"),
        P(),
        P(None, "tp"),
        P(None, "tp"),
        P(None, "tp"),
        P(None, "tp"),
        P(None, "tp"),
        P("tp"),
        P(None, "tp"),
        P(),
        P(None, "tp"),
        P(None, "tp"),
        P(None, "tp"),
        P(None, "tp"),
    )
    out_specs = (P("sp", "tp"), P("tp", "sp"))
    return jax.shard_map(body, mesh=mesh, in_specs=in_specs, out_specs=out_specs, check_vma=False)
```

```python
import functools

import jax
import jax.numpy as jnp
from jax import lax
from jax.experimental import pallas as pl
from jax.experimental.pallas import tpu as pltpu
from jax.sharding import PartitionSpec as P

HEAD = 64
WIDTH = 31
LANES = 128
HALO = 32
MESH = pl.DeviceIdType.MESH


key_span = 512


def passed_along(array, axis, by):
    length = lax.axis_size(axis)
    pairs = [(i, i + by) for i in range(length) if 0 <= i + by < length]
    return lax.ppermute(array, axis, pairs)


def sweep_block(
    sweep_state, key_block, value_block, key_first, query_first, query_heads, offsets, score_scale
):
    summed, spent_stick = sweep_state
    head_count = offsets.shape[0]
    query_count = query_heads.shape[0]
    key_count = key_block.shape[0]
    key_heads = key_block.reshape(key_count, head_count, -1)
    value_heads = value_block.reshape(key_count, head_count, -1)
    scores = (
        jnp.einsum("thd,shd->hts", query_heads, key_heads, preferred_element_type=jnp.float32)
        * score_scale
        + offsets[:, None, None]
    )
    query_pos = query_first + lax.iota(jnp.int32, query_count)
    key_pos = key_first + lax.iota(jnp.int32, key_count)
    allowed = (key_pos[None, :] <= query_pos[:, None]) & (key_pos[None, :] >= 0)
    softened = jnp.where(allowed[None], jax.nn.softplus(scores), 0.0)
    behind = lax.cumsum(softened, axis=2, reverse=True)
    stick = jnp.where(
        allowed[None], jnp.exp(scores - behind - spent_stick[:, :, None]), 0.0
    ).astype(jnp.bfloat16)
    summed = summed + jnp.einsum(
        "hts,shd->thd", stick, value_heads, preferred_element_type=jnp.float32
    )
    return (summed, spent_stick + behind[:, :, 0])


def plain_body(
    tokens,
    norm_gain,
    w_glu_value,
    w_glu_gate,
    w_query,
    w_key,
    w_value,
    score_offset,
    conv_taps,
    conv_gain,
    w_conv_out,
    w_attn_out,
    w_gate_conv,
    w_gate_attn,
):
    whole_rows = lax.all_gather(tokens, "tp", axis=1, tiled=True)
    features = whole_rows.astype(jnp.float32)
    normed = (
        features
        * lax.rsqrt(jnp.mean(features * features, axis=-1, keepdims=True) + 1e-06)
        * norm_gain
    ).astype(jnp.bfloat16)
    glued = (
        jnp.dot(normed, w_glu_value, preferred_element_type=jnp.float32)
        * jax.nn.sigmoid(jnp.dot(normed, w_glu_gate, preferred_element_type=jnp.float32))
    ).astype(jnp.bfloat16)
    queries = jnp.dot(normed, w_query, preferred_element_type=jnp.float32).astype(jnp.bfloat16)
    keys = jnp.dot(normed, w_key, preferred_element_type=jnp.float32).astype(jnp.bfloat16)
    values = jnp.dot(normed, w_value, preferred_element_type=jnp.float32).astype(jnp.bfloat16)
    tok_rows = whole_rows.shape[0]
    tap_count = conv_taps.shape[0]
    channels = glued.shape[1]
    previous = passed_along(glued[tok_rows - (tap_count - 1) :], "sp", 1)
    extended = jnp.concatenate([previous, glued], axis=0)
    tap_rows = conv_taps.astype(jnp.float32)
    convolved = jnp.zeros((tok_rows, channels), jnp.float32)
    for tap in range(WIDTH):
        convolved = convolved + tap_rows[tap] * extended[tap : tap + tok_rows].astype(jnp.float32)
    convolved = convolved.astype(jnp.bfloat16)
    head_count = score_offset.shape[0]
    head_width = queries.shape[1] // head_count
    score_scale = 1.0 / HEAD**0.5
    query_heads = queries.reshape(tok_rows, head_count, head_width)
    own_index = lax.axis_index("sp")
    query_first = own_index * tok_rows
    start_state = (
        jnp.zeros((tok_rows, head_count, head_width), jnp.float32),
        jnp.zeros((head_count, tok_rows), jnp.float32),
    )
    gathered = (
        lax.all_gather(keys, "sp", axis=0, tiled=True),
        lax.all_gather(values, "sp", axis=0, tiled=True),
    )
    leading = jnp.zeros((key_span, keys.shape[1]), jnp.bfloat16)
    all_keys = jnp.concatenate([leading, gathered[0]], axis=0)
    all_values = jnp.concatenate([leading, gathered[1]], axis=0)
    key_end = (own_index + 1) * tok_rows
    turns = (key_end + key_span - 1) // key_span

    def advance(turn_index, sweep_state):
        key_first = key_end - (turn_index + 1) * key_span
        key_block = lax.dynamic_slice_in_dim(all_keys, key_first + key_span, key_span, 0)
        value_block = lax.dynamic_slice_in_dim(all_values, key_first + key_span, key_span, 0)
        return sweep_block(
            sweep_state,
            key_block,
            value_block,
            key_first,
            query_first,
            query_heads,
            score_offset,
            score_scale,
        )

    summed, spent_stick = lax.fori_loop(0, turns, advance, start_state)
    attended = summed.reshape(tok_rows, head_count * head_width).astype(jnp.bfloat16)
    log_weight = jnp.log(-jnp.expm1(-spent_stick))
    gate_conv = jax.nn.sigmoid(jnp.dot(normed, w_gate_conv, preferred_element_type=jnp.float32))
    gate_attn = jax.nn.sigmoid(jnp.dot(normed, w_gate_attn, preferred_element_type=jnp.float32))
    all_channels = conv_gain.shape[0]
    conv_float = convolved.astype(jnp.float32)
    channel_sum, channel_squares = lax.psum(
        (
            jnp.sum(conv_float, axis=-1, keepdims=True),
            jnp.sum(conv_float * conv_float, axis=-1, keepdims=True),
        ),
        "tp",
    )
    channel_mean = channel_sum / all_channels
    channel_var = channel_squares / all_channels - channel_mean * channel_mean
    local_gain = lax.dynamic_slice_in_dim(conv_gain, lax.axis_index("tp") * channels, channels, 0)
    conv_act = jax.nn.silu(
        (conv_float - channel_mean) * lax.rsqrt(channel_var + 1e-05) * local_gain
    ).astype(jnp.bfloat16)
    conv_piece = lax.all_gather(conv_act, "tp", axis=1, tiled=True)
    attn_piece = lax.all_gather(attended, "tp", axis=1, tiled=True)
    conv_branch = jnp.dot(conv_piece, w_conv_out, preferred_element_type=jnp.float32)
    attn_branch = jnp.dot(attn_piece, w_attn_out, preferred_element_type=jnp.float32)
    mixed = (gate_conv * conv_branch + gate_attn * attn_branch).astype(jnp.bfloat16)
    return (mixed, log_weight)


def remote(src, dst, send_sem, recv_sem, where):
    return pltpu.make_async_remote_copy(
        src_ref=src, dst_ref=dst, send_sem=send_sem, recv_sem=recv_sem,
        device_id=where, device_id_type=MESH,
    )


class Spread:
    def __init__(self, own_ref, whole_ref, send_sem, recv_sem, pass_send, pass_recv):
        self.count = lax.axis_size("tp")
        self.me = lax.axis_index("tp")
        self.partner = self.me + 1 - 2 * (self.me % 2)
        self.own_ref, self.whole_ref = own_ref, whole_ref
        self.sems = (send_sem, recv_sem, pass_send, pass_recv)
        self.far = range(1, self.count // 2)

    def columns(self, index):
        width = self.own_ref.shape[1]
        return self.whole_ref.at[:, pl.ds(pl.multiple_of(index * width, width), width)]

    def first(self, step):
        where = self.partner if step == 0 else (self.me + 2 * step) % self.count
        return remote(
            self.own_ref, self.columns(self.me), self.sems[0].at[step], self.sems[1].at[step],
            {"tp": where},
        )

    def passing(self, step):
        held = self.columns((self.me - 2 * step + self.count) % self.count)
        return remote(
            held, held, self.sems[2].at[step], self.sems[3].at[step], {"tp": self.partner}
        )

    def start(self):
        for step in self.far:
            self.first(step).start()
        self.first(0).start()

    def forward(self):
        for step in self.far:
            self.first(step).wait_recv()
            self.passing(step).start()

    def finish(self):
        self.first(0).wait()
        for step in self.far:
            self.first(step).wait_send()
            self.passing(step).wait()

    @staticmethod
    def semaphores(count):
        return [pltpu.SemaphoreType.DMA((count // 2,)) for _ in range(4)]


def greet(barrier):
    tp_count, tp_me = lax.axis_size("tp"), lax.axis_index("tp")
    others = [{"tp": tp_me + 1 - 2 * (tp_me % 2)}]
    others += [{"tp": (tp_me + 2 * step) % tp_count} for step in range(1, tp_count // 2)]
    for other in others:
        pl.semaphore_signal(barrier, inc=1, device_id=other, device_id_type=MESH)
    pl.semaphore_wait(barrier, len(others))


def token_kernel(own_ref, gain_ref, normed_ref, whole_ref, keep_sem, *sems):
    spread = Spread(own_ref, whole_ref, *sems)
    greet(pltpu.get_barrier_semaphore())
    spread.start()
    keep = pltpu.make_async_copy(own_ref, spread.columns(spread.me), keep_sem)
    keep.start()
    spread.forward()
    keep.wait()
    spread.finish()
    features_count = whole_ref.shape[1]
    tall = 64

    @pl.loop(0, whole_ref.shape[0] // tall)
    def _(index):
        rows = pl.ds(pl.multiple_of(index * tall, tall), tall)
        features = whole_ref[rows, :].astype(jnp.float32)
        square = jnp.sum(features * features, axis=-1, keepdims=True) / features_count
        normed_ref[rows, :] = (features * lax.rsqrt(square + 1e-06) * gain_ref[...]).astype(
            jnp.bfloat16
        )


def gather_normed(tokens, norm_gain):
    rows, columns = tokens.shape
    count = lax.axis_size("tp")
    return pl.pallas_call(
        token_kernel,
        in_specs=[pl.BlockSpec(memory_space=pltpu.VMEM)] * 2,
        out_specs=pl.BlockSpec(memory_space=pltpu.VMEM),
        out_shape=jax.ShapeDtypeStruct((rows, columns * count), jnp.bfloat16),
        scratch_shapes=[
            pltpu.VMEM((rows, columns * count), jnp.bfloat16), pltpu.SemaphoreType.DMA
        ] + Spread.semaphores(count),
        compiler_params=pltpu.CompilerParams(
            collective_id=0, has_side_effects=True, vmem_limit_bytes=16 << 20
        ),
    )(tokens, norm_gain[None])


def softplus_parts(z):
    x = jnp.exp(-jnp.abs(z))
    tail = jnp.where(x < 0.004, x - (0.5 * x) * x, jnp.log(1.0 + x))
    return jnp.maximum(z, 0.0) + tail, jnp.minimum(z, 0.0) - tail


def branch_kernel(
    tap_count, scale, offset_ref, packed_ref, normed_ref, value_hbm, gate_hbm, taps_ref, gain_ref,
    act_ref, attended_ref, spent_ref,
    chunks, key_s, value_s, query_s, acc_s, carry_s,
    back_out, back_in, spent_out, spent_in, own_rows,
    value_w, gate_w, glued_s, halo_s, extended, conv_s, own_act, stat_out, stat_in,
    weight_sem, keep_sem, chunk_send, chunk_recv, back_send, back_recv, spent_send, spent_recv,
    halo_send, halo_recv, stat_send, stat_recv, *spread_sems
):
    sp_count, me = lax.axis_size("sp"), lax.axis_index("sp")
    tp_count, tp_me = lax.axis_size("tp"), lax.axis_index("tp")
    rows, channels = own_rows.shape
    width = packed_ref.shape[2] // 3
    cell = LANES

    weights = [
        pltpu.make_async_copy(hbm, vmem, weight_sem.at[index])
        for index, (hbm, vmem) in enumerate(((value_hbm, value_w), (gate_hbm, gate_w)))
    ]
    for copy in weights:
        copy.start()
    barrier = pltpu.get_barrier_semaphore()
    for step in range(1, sp_count):
        pl.semaphore_signal(
            barrier, inc=1, device_id={"sp": (me + step) % sp_count}, device_id_type=MESH
        )
    for step in range(1, tp_count):
        pl.semaphore_signal(
            barrier, inc=1, device_id={"tp": (tp_me + step) % tp_count}, device_id_type=MESH
        )
    pl.semaphore_wait(barrier, sp_count + tp_count - 2)

    def chunk_copy(step):
        to = (me + step) % sp_count
        return remote(
            packed_ref.at[to], chunks.at[me], chunk_send.at[step], chunk_recv.at[step], {"sp": to}
        )

    for step in range(1, sp_count):
        chunk_copy(step).start()
    keep = pltpu.make_async_copy(packed_ref.at[me], chunks.at[me], keep_sem)
    keep.start()

    for copy in weights:
        copy.wait()
    part = 2 * LANES if channels % (2 * LANES) == 0 else channels
    for first in range(0, channels, part):
        cols = pl.ds(first, part)
        value = jnp.dot(normed_ref[...], value_w[:, cols], preferred_element_type=jnp.float32)
        gate = jnp.dot(normed_ref[...], gate_w[:, cols], preferred_element_type=jnp.float32)
        glued = (value * jax.nn.sigmoid(gate)).astype(jnp.bfloat16)
        extended[pl.ds(HALO, rows), cols] = glued.astype(jnp.float32)
        glued_s[:, cols] = glued[rows - HALO :]

    def halo_copy():
        return remote(
            glued_s, halo_s, halo_send, halo_recv, {"sp": (me + 1) % sp_count}
        )

    @pl.when(me < sp_count - 1)
    def _():
        halo_copy().start()

    @pl.when(me == 0)
    def _():
        extended[pl.ds(0, HALO), :] = jnp.zeros((HALO, channels), jnp.float32)

    @pl.when(me > 0)
    def _():
        halo_copy().wait_recv()
        extended[pl.ds(0, HALO), :] = halo_s[...].astype(jnp.float32)

    carry_s[...] = jnp.zeros_like(carry_s)
    acc_s[...] = jnp.zeros_like(acc_s)
    sums = [jnp.zeros((rows, 1), jnp.float32)] * 2
    for first in range(0, channels, LANES):
        cols = pl.ds(first, LANES)
        conv = jnp.zeros((rows, LANES), jnp.float32)
        for tap in range(tap_count):
            weight = taps_ref[tap : tap + 1, cols].astype(jnp.float32)
            conv = conv + weight * extended[pl.ds(HALO - tap_count + 1 + tap, rows), cols]
        conv = conv.astype(jnp.bfloat16)
        conv_s[:, cols] = conv
        conv = conv.astype(jnp.float32)
        sums = [
            sums[0] + jnp.sum(conv, axis=1, keepdims=True),
            sums[1] + jnp.sum(conv * conv, axis=1, keepdims=True),
        ]
    for index in range(2):
        stat_out[8 * index : 8 * index + 8, :] = jnp.transpose(
            jnp.broadcast_to(sums[index], (rows, LANES))
        )[:8]

    def stat_copy(step):
        return remote(
            stat_out, stat_in.at[step], stat_send.at[step], stat_recv.at[step],
            {"tp": (tp_me + step) % tp_count},
        )

    for step in range(1, tp_count):
        stat_copy(step).start()
    total = stat_out[...]
    for step in range(1, tp_count):
        stat_copy(step).wait_recv()
        total = total + stat_in[step]
    all_channels = channels * tp_count
    mean = jnp.transpose(jnp.broadcast_to(total[:1], (LANES, rows))) / all_channels
    square = jnp.transpose(jnp.broadcast_to(total[8:9], (LANES, rows))) / all_channels
    inverse = lax.rsqrt(square - mean * mean + 1e-05)
    for first in range(0, channels, LANES):
        cols = pl.ds(first, LANES)
        act = (conv_s[:, cols].astype(jnp.float32) - mean) * inverse * gain_ref[:, cols]
        own_act[:, cols] = (act * jax.nn.sigmoid(act)).astype(jnp.bfloat16)

    act_spread = Spread(own_act, act_ref, *spread_sems[:4])
    act_spread.start()
    act_keep = pltpu.make_async_copy(own_act, act_spread.columns(tp_me), keep_sem)
    keep.wait()
    act_keep.start()
    act_keep.wait()

    offset = offset_ref[0, me]
    side = lax.broadcasted_iota(jnp.int32, (cell, 2 * cell), 0)
    across = lax.broadcasted_iota(jnp.int32, (cell, 2 * cell), 1)
    later = ((side > across) | (across >= cell)).astype(jnp.bfloat16)

    def one(row, key_block, col, diagonal):
        held = pl.ds(row, rows - row)
        z = (
            lax.dot_general(
                query_s[held, :], key_s[key_block, pl.ds(col, cell), :],
                (((1,), (1,)), ((), ())), preferred_element_type=jnp.float32,
            )
            * scale
            + offset
        )
        soft, own = softplus_parts(z)
        if diagonal:
            allowed = lax.broadcasted_iota(jnp.int32, z.shape, 1) <= lax.broadcasted_iota(
                jnp.int32, z.shape, 0
            )
            soft = jnp.where(allowed, soft, 0.0)
        behind = jnp.dot(soft.astype(jnp.bfloat16), later, preferred_element_type=jnp.float32)
        carry = carry_s[held, :]
        stick = jnp.exp(own - behind[:, :cell] - carry)
        if diagonal:
            stick = jnp.where(allowed, stick, 0.0)
        acc_s[held, :] += jnp.dot(
            stick.astype(jnp.bfloat16), value_s[key_block, pl.ds(col, cell), :],
            preferred_element_type=jnp.float32,
        )
        carry_s[held, :] = carry + behind[:, cell:]

    def back_copies(to, source):
        return (
            remote(
                back_out.at[to], back_in.at[source], back_send.at[to], back_recv.at[source],
                {"sp": to},
            ),
            remote(
                spent_out.at[to], spent_in.at[source], spent_send.at[to], spent_recv.at[source],
                {"sp": to},
            ),
        )

    def block(index, _):
        @pl.when(index != me)
        def _():
            step = (me - index + sp_count) % sp_count
            remote(
                packed_ref.at[index], chunks.at[index], chunk_send.at[step], chunk_recv.at[step],
                {"sp": (me + step) % sp_count},
            ).wait_recv()

        @pl.when(index == sp_count // 2)
        def _():
            act_spread.forward()

        query_s[...] = chunks[index, :, :width]
        key_s[index] = chunks[index, :, width : 2 * width]
        value_s[index] = chunks[index, :, 2 * width :]
        acc_s[...] = jnp.zeros_like(acc_s)
        carry_s[...] = jnp.zeros_like(carry_s)
        for col in range(rows - cell, -1, -cell):
            one(col, index, col, True)

        def turn(back, _):
            for col in range(rows - cell, -1, -cell):
                one(0, index - 1 - back, col, False)
            return 0

        lax.fori_loop(0, index, turn, 0)
        done = acc_s[...].astype(jnp.bfloat16)
        spent = jnp.transpose(carry_s[...])[:8]

        @pl.when(index != me)
        def _():
            back_out[index] = done
            spent_out[index] = spent
            for copy in back_copies(index, me):
                copy.start()

        @pl.when(index == me)
        def _():
            back_in[index] = done
            spent_in[index] = spent

        return 0

    lax.fori_loop(0, sp_count, block, 0)

    for source in range(sp_count):
        @pl.when(source != me)
        def _():
            for copy in back_copies((2 * me - source + sp_count) % sp_count, source):
                copy.wait_recv()
    own_rows[...] = jnp.concatenate([back_in[source] for source in range(sp_count)], axis=1)
    last_spread = Spread(own_rows, attended_ref, *spread_sems[4:])
    last_spread.start()
    last_keep = pltpu.make_async_copy(own_rows, last_spread.columns(tp_me), keep_sem)
    last_keep.start()
    for source in range(sp_count):
        spent_ref[source : source + 1, :] = spent_in[source, :1]
    for step in range(1, sp_count):
        chunk_copy(step).wait_send()
        for copy in back_copies((me + step) % sp_count, me):
            copy.wait_send()
    for step in range(1, tp_count):
        stat_copy(step).wait_send()

    @pl.when(me < sp_count - 1)
    def _():
        halo_copy().wait_send()

    act_spread.finish()
    last_keep.wait()
    last_spread.forward()
    last_spread.finish()


def branches(packed, normed, w_value, w_gate, taps, gain, offsets, scale):
    sp_count, rows, wide = packed.shape
    width = wide // 3
    tp_count = lax.axis_size("tp")
    channels = taps.shape[1]
    bf, f32 = jnp.bfloat16, jnp.float32
    dma = pltpu.SemaphoreType.DMA
    vmem = pl.BlockSpec(memory_space=pltpu.VMEM)
    hbm = pl.BlockSpec(memory_space=pl.ANY)
    return pl.pallas_call(
        functools.partial(branch_kernel, taps.shape[0], scale),
        in_specs=[pl.BlockSpec(memory_space=pltpu.SMEM), vmem, vmem, hbm, hbm, vmem, vmem],
        out_specs=[vmem, vmem, vmem],
        out_shape=[
            jax.ShapeDtypeStruct((rows, channels * tp_count), bf),
            jax.ShapeDtypeStruct((rows, channels * tp_count), bf),
            jax.ShapeDtypeStruct((sp_count, rows), f32),
        ],
        scratch_shapes=[
            pltpu.VMEM((sp_count, rows, wide), bf),
            pltpu.VMEM((sp_count, rows, width), bf),
            pltpu.VMEM((sp_count, rows, width), bf),
            pltpu.VMEM((rows, width), bf),
            pltpu.VMEM((rows, width), f32),
            pltpu.VMEM((rows, LANES), f32),
            pltpu.VMEM((sp_count, rows, width), bf),
            pltpu.VMEM((sp_count, rows, width), bf),
            pltpu.VMEM((sp_count, 8, rows), f32),
            pltpu.VMEM((sp_count, 8, rows), f32),
            pltpu.VMEM((rows, channels), bf),
            pltpu.VMEM(w_value.shape, bf),
            pltpu.VMEM(w_gate.shape, bf),
            pltpu.VMEM((HALO, channels), bf),
            pltpu.VMEM((HALO, channels), bf),
            pltpu.VMEM((HALO + rows, channels), f32),
            pltpu.VMEM((rows, channels), bf),
            pltpu.VMEM((rows, channels), bf),
            pltpu.VMEM((16, rows), f32),
            pltpu.VMEM((tp_count, 16, rows), f32),
            dma((2,)), dma,
            dma((sp_count,)), dma((sp_count,)), dma((sp_count,)), dma((sp_count,)),
            dma((sp_count,)), dma((sp_count,)), dma, dma, dma((tp_count,)), dma((tp_count,)),
        ] + Spread.semaphores(tp_count) + Spread.semaphores(tp_count),
        compiler_params=pltpu.CompilerParams(
            collective_id=1, has_side_effects=True, vmem_limit_bytes=48 << 20
        ),
        cost_estimate=pl.CostEstimate(
            flops=4 * sp_count * sp_count * rows * rows * width,
            bytes_accessed=8 * w_value.size,
            transcendentals=2 * sp_count * sp_count * rows * rows,
        ),
    )(offsets, packed, normed, w_value, w_gate, taps, gain)


def body(
    tokens, norm_gain, w_glu_value, w_glu_gate, w_query, w_key, w_value, score_offset, conv_taps,
    conv_gain, w_conv_out, w_attn_out, w_gate_conv, w_gate_attn,
):
    sp_count, tp_count = lax.axis_size("sp"), lax.axis_size("tp")
    rows, channels = tokens.shape[0], w_query.shape[1]
    head_count = score_offset.shape[0]
    fits = rows % LANES == 0 and channels % LANES == 0 and conv_taps.shape[0] <= HALO + 1
    if head_count != sp_count or tp_count % 2 or not fits:
        return plain_body(
            tokens, norm_gain, w_glu_value, w_glu_gate, w_query, w_key, w_value, score_offset,
            conv_taps, conv_gain, w_conv_out, w_attn_out, w_gate_conv, w_gate_attn,
        )
    width = channels // head_count
    normed = gather_normed(tokens, norm_gain)
    packed = jnp.stack(
        [
            jnp.dot(normed, weight, preferred_element_type=jnp.float32)
            .astype(jnp.bfloat16)
            .reshape(rows, sp_count, width)
            for weight in (w_query, w_key, w_value)
        ],
        axis=2,
    ).reshape(rows, sp_count, 3 * width).transpose(1, 0, 2)
    local_gain = lax.dynamic_slice_in_dim(conv_gain, lax.axis_index("tp") * channels, channels, 0)
    conv_piece, attn_piece, spent_stick = branches(
        packed, normed, w_glu_value, w_glu_gate, conv_taps, local_gain[None], score_offset[None],
        1.0 / width**0.5,
    )
    log_weight = jnp.log(-jnp.expm1(-spent_stick))
    gate_conv = jax.nn.sigmoid(jnp.dot(normed, w_gate_conv, preferred_element_type=jnp.float32))
    gate_attn = jax.nn.sigmoid(jnp.dot(normed, w_gate_attn, preferred_element_type=jnp.float32))
    conv_branch = jnp.dot(conv_piece, w_conv_out, preferred_element_type=jnp.float32)
    attn_branch = jnp.dot(attn_piece, w_attn_out, preferred_element_type=jnp.float32)
    mixed = (gate_conv * conv_branch + gate_attn * attn_branch).astype(jnp.bfloat16)
    return (mixed, log_weight)


def solution(mesh):
    in_specs = (
        P("sp", "tp"),
        P(),
        P(None, "tp"),
        P(None, "tp"),
        P(None, "tp"),
        P(None, "tp"),
        P(None, "tp"),
        P("tp"),
        P(None, "tp"),
        P(),
        P(None, "tp"),
        P(None, "tp"),
        P(None, "tp"),
        P(None, "tp"),
    )
    out_specs = (P("sp", "tp"), P("tp", "sp"))
    return jax.shard_map(body, mesh=mesh, in_specs=in_specs, out_specs=out_specs, check_vma=False)
```

```python
import functools

import jax
import jax.numpy as jnp
from jax import lax
from jax.experimental import pallas as pl
from jax.experimental.pallas import tpu as pltpu
from jax.sharding import PartitionSpec as P

HEAD = 64
WIDTH = 31
LANES = 128
HALO = 32
MESH = pl.DeviceIdType.MESH


key_span = 512


def passed_along(array, axis, by):
    length = lax.axis_size(axis)
    pairs = [(i, i + by) for i in range(length) if 0 <= i + by < length]
    return lax.ppermute(array, axis, pairs)


def sweep_block(
    sweep_state, key_block, value_block, key_first, query_first, query_heads, offsets, score_scale
):
    summed, spent_stick = sweep_state
    head_count = offsets.shape[0]
    query_count = query_heads.shape[0]
    key_count = key_block.shape[0]
    key_heads = key_block.reshape(key_count, head_count, -1)
    value_heads = value_block.reshape(key_count, head_count, -1)
    scores = (
        jnp.einsum("thd,shd->hts", query_heads, key_heads, preferred_element_type=jnp.float32)
        * score_scale
        + offsets[:, None, None]
    )
    query_pos = query_first + lax.iota(jnp.int32, query_count)
    key_pos = key_first + lax.iota(jnp.int32, key_count)
    allowed = (key_pos[None, :] <= query_pos[:, None]) & (key_pos[None, :] >= 0)
    softened = jnp.where(allowed[None], jax.nn.softplus(scores), 0.0)
    behind = lax.cumsum(softened, axis=2, reverse=True)
    stick = jnp.where(
        allowed[None], jnp.exp(scores - behind - spent_stick[:, :, None]), 0.0
    ).astype(jnp.bfloat16)
    summed = summed + jnp.einsum(
        "hts,shd->thd", stick, value_heads, preferred_element_type=jnp.float32
    )
    return (summed, spent_stick + behind[:, :, 0])


def plain_body(
    tokens,
    norm_gain,
    w_glu_value,
    w_glu_gate,
    w_query,
    w_key,
    w_value,
    score_offset,
    conv_taps,
    conv_gain,
    w_conv_out,
    w_attn_out,
    w_gate_conv,
    w_gate_attn,
):
    whole_rows = lax.all_gather(tokens, "tp", axis=1, tiled=True)
    features = whole_rows.astype(jnp.float32)
    normed = (
        features
        * lax.rsqrt(jnp.mean(features * features, axis=-1, keepdims=True) + 1e-06)
        * norm_gain
    ).astype(jnp.bfloat16)
    glued = (
        jnp.dot(normed, w_glu_value, preferred_element_type=jnp.float32)
        * jax.nn.sigmoid(jnp.dot(normed, w_glu_gate, preferred_element_type=jnp.float32))
    ).astype(jnp.bfloat16)
    queries = jnp.dot(normed, w_query, preferred_element_type=jnp.float32).astype(jnp.bfloat16)
    keys = jnp.dot(normed, w_key, preferred_element_type=jnp.float32).astype(jnp.bfloat16)
    values = jnp.dot(normed, w_value, preferred_element_type=jnp.float32).astype(jnp.bfloat16)
    tok_rows = whole_rows.shape[0]
    tap_count = conv_taps.shape[0]
    channels = glued.shape[1]
    previous = passed_along(glued[tok_rows - (tap_count - 1) :], "sp", 1)
    extended = jnp.concatenate([previous, glued], axis=0)
    tap_rows = conv_taps.astype(jnp.float32)
    convolved = jnp.zeros((tok_rows, channels), jnp.float32)
    for tap in range(WIDTH):
        convolved = convolved + tap_rows[tap] * extended[tap : tap + tok_rows].astype(jnp.float32)
    convolved = convolved.astype(jnp.bfloat16)
    head_count = score_offset.shape[0]
    head_width = queries.shape[1] // head_count
    score_scale = 1.0 / HEAD**0.5
    query_heads = queries.reshape(tok_rows, head_count, head_width)
    own_index = lax.axis_index("sp")
    query_first = own_index * tok_rows
    start_state = (
        jnp.zeros((tok_rows, head_count, head_width), jnp.float32),
        jnp.zeros((head_count, tok_rows), jnp.float32),
    )
    gathered = (
        lax.all_gather(keys, "sp", axis=0, tiled=True),
        lax.all_gather(values, "sp", axis=0, tiled=True),
    )
    leading = jnp.zeros((key_span, keys.shape[1]), jnp.bfloat16)
    all_keys = jnp.concatenate([leading, gathered[0]], axis=0)
    all_values = jnp.concatenate([leading, gathered[1]], axis=0)
    key_end = (own_index + 1) * tok_rows
    turns = (key_end + key_span - 1) // key_span

    def advance(turn_index, sweep_state):
        key_first = key_end - (turn_index + 1) * key_span
        key_block = lax.dynamic_slice_in_dim(all_keys, key_first + key_span, key_span, 0)
        value_block = lax.dynamic_slice_in_dim(all_values, key_first + key_span, key_span, 0)
        return sweep_block(
            sweep_state,
            key_block,
            value_block,
            key_first,
            query_first,
            query_heads,
            score_offset,
            score_scale,
        )

    summed, spent_stick = lax.fori_loop(0, turns, advance, start_state)
    attended = summed.reshape(tok_rows, head_count * head_width).astype(jnp.bfloat16)
    log_weight = jnp.log(-jnp.expm1(-spent_stick))
    gate_conv = jax.nn.sigmoid(jnp.dot(normed, w_gate_conv, preferred_element_type=jnp.float32))
    gate_attn = jax.nn.sigmoid(jnp.dot(normed, w_gate_attn, preferred_element_type=jnp.float32))
    all_channels = conv_gain.shape[0]
    conv_float = convolved.astype(jnp.float32)
    channel_sum, channel_squares = lax.psum(
        (
            jnp.sum(conv_float, axis=-1, keepdims=True),
            jnp.sum(conv_float * conv_float, axis=-1, keepdims=True),
        ),
        "tp",
    )
    channel_mean = channel_sum / all_channels
    channel_var = channel_squares / all_channels - channel_mean * channel_mean
    local_gain = lax.dynamic_slice_in_dim(conv_gain, lax.axis_index("tp") * channels, channels, 0)
    conv_act = jax.nn.silu(
        (conv_float - channel_mean) * lax.rsqrt(channel_var + 1e-05) * local_gain
    ).astype(jnp.bfloat16)
    conv_piece = lax.all_gather(conv_act, "tp", axis=1, tiled=True)
    attn_piece = lax.all_gather(attended, "tp", axis=1, tiled=True)
    conv_branch = jnp.dot(conv_piece, w_conv_out, preferred_element_type=jnp.float32)
    attn_branch = jnp.dot(attn_piece, w_attn_out, preferred_element_type=jnp.float32)
    mixed = (gate_conv * conv_branch + gate_attn * attn_branch).astype(jnp.bfloat16)
    return (mixed, log_weight)


def remote(src, dst, send_sem, recv_sem, where):
    return pltpu.make_async_remote_copy(
        src_ref=src, dst_ref=dst, send_sem=send_sem, recv_sem=recv_sem,
        device_id=where, device_id_type=MESH,
    )


class Spread:
    def __init__(self, own_ref, whole_ref, send_sem, recv_sem, pass_send, pass_recv):
        self.count = lax.axis_size("tp")
        self.me = lax.axis_index("tp")
        self.partner = self.me + 1 - 2 * (self.me % 2)
        self.own_ref, self.whole_ref = own_ref, whole_ref
        self.sems = (send_sem, recv_sem, pass_send, pass_recv)
        self.far = range(1, self.count // 2)

    def columns(self, index):
        width = self.own_ref.shape[1]
        return self.whole_ref.at[:, pl.ds(pl.multiple_of(index * width, width), width)]

    def first(self, step):
        where = self.partner if step == 0 else (self.me + 2 * step) % self.count
        return remote(
            self.own_ref, self.columns(self.me), self.sems[0].at[step], self.sems[1].at[step],
            {"tp": where},
        )

    def passing(self, step):
        held = self.columns((self.me - 2 * step + self.count) % self.count)
        return remote(
            held, held, self.sems[2].at[step], self.sems[3].at[step], {"tp": self.partner}
        )

    def start(self):
        for step in self.far:
            self.first(step).start()
        self.first(0).start()

    def forward(self):
        for step in self.far:
            self.first(step).wait_recv()
            self.passing(step).start()

    def finish(self):
        self.first(0).wait()
        for step in self.far:
            self.first(step).wait_send()
            self.passing(step).wait()

    @staticmethod
    def semaphores(count):
        return [pltpu.SemaphoreType.DMA((count // 2,)) for _ in range(4)]


def greet(barrier):
    tp_count, tp_me = lax.axis_size("tp"), lax.axis_index("tp")
    others = [{"tp": tp_me + 1 - 2 * (tp_me % 2)}]
    others += [{"tp": (tp_me + 2 * step) % tp_count} for step in range(1, tp_count // 2)]
    for other in others:
        pl.semaphore_signal(barrier, inc=1, device_id=other, device_id_type=MESH)
    pl.semaphore_wait(barrier, len(others))


def token_kernel(own_ref, gain_ref, normed_ref, whole_ref, keep_sem, *sems):
    spread = Spread(own_ref, whole_ref, *sems)
    greet(pltpu.get_barrier_semaphore())
    spread.start()
    keep = pltpu.make_async_copy(own_ref, spread.columns(spread.me), keep_sem)
    keep.start()
    spread.forward()
    keep.wait()
    spread.finish()
    features_count = whole_ref.shape[1]
    tall = 64

    @pl.loop(0, whole_ref.shape[0] // tall)
    def _(index):
        rows = pl.ds(pl.multiple_of(index * tall, tall), tall)
        features = whole_ref[rows, :].astype(jnp.float32)
        square = jnp.sum(features * features, axis=-1, keepdims=True) / features_count
        normed_ref[rows, :] = (features * lax.rsqrt(square + 1e-06) * gain_ref[...]).astype(
            jnp.bfloat16
        )


def gather_normed(tokens, norm_gain):
    rows, columns = tokens.shape
    count = lax.axis_size("tp")
    return pl.pallas_call(
        token_kernel,
        in_specs=[pl.BlockSpec(memory_space=pltpu.VMEM)] * 2,
        out_specs=pl.BlockSpec(memory_space=pltpu.VMEM),
        out_shape=jax.ShapeDtypeStruct((rows, columns * count), jnp.bfloat16),
        scratch_shapes=[
            pltpu.VMEM((rows, columns * count), jnp.bfloat16), pltpu.SemaphoreType.DMA
        ] + Spread.semaphores(count),
        compiler_params=pltpu.CompilerParams(
            collective_id=0, has_side_effects=True, vmem_limit_bytes=16 << 20
        ),
    )(tokens, norm_gain[None])


def softplus_parts(z):
    x = jnp.exp(-jnp.abs(z))
    tail = jnp.where(x < 0.004, x - (0.5 * x) * x, jnp.log(1.0 + x))
    return jnp.maximum(z, 0.0) + tail, jnp.minimum(z, 0.0) - tail


def branch_kernel(
    tap_count, scale, offset_ref, packed_ref, normed_ref, value_hbm, gate_hbm, taps_ref, gain_ref,
    act_ref, attended_ref, spent_ref,
    chunks, key_s, value_s, query_s, acc_s, carry_s,
    back_out, back_in, spent_out, spent_in, own_rows,
    value_w, gate_w, glued_s, halo_s, extended, conv_s, own_act, stat_out, stat_in,
    weight_sem, keep_sem, chunk_send, chunk_recv, back_send, back_recv, spent_send, spent_recv,
    halo_send, halo_recv, stat_send, stat_recv, *spread_sems
):
    sp_count, me = lax.axis_size("sp"), lax.axis_index("sp")
    tp_count, tp_me = lax.axis_size("tp"), lax.axis_index("tp")
    rows, channels = own_rows.shape
    width = packed_ref.shape[2] // 2
    half = rows // 2
    cell = LANES

    weights = [
        pltpu.make_async_copy(hbm, vmem, weight_sem.at[index])
        for index, (hbm, vmem) in enumerate(((value_hbm, value_w), (gate_hbm, gate_w)))
    ]
    for copy in weights:
        copy.start()
    barrier = pltpu.get_barrier_semaphore()
    for step in range(1, sp_count):
        pl.semaphore_signal(
            barrier, inc=1, device_id={"sp": (me + step) % sp_count}, device_id_type=MESH
        )
    for step in range(1, tp_count):
        pl.semaphore_signal(
            barrier, inc=1, device_id={"tp": (tp_me + step) % tp_count}, device_id_type=MESH
        )
    pl.semaphore_wait(barrier, sp_count + tp_count - 2)

    def chunk_copy(step):
        to = (me + step) % sp_count
        return remote(
            packed_ref.at[to], chunks.at[me], chunk_send.at[step], chunk_recv.at[step], {"sp": to}
        )

    for step in sorted(range(1, sp_count), key=lambda step: abs(step - sp_count // 2)):
        chunk_copy(step).start()
    keep = pltpu.make_async_copy(packed_ref.at[me], chunks.at[me], keep_sem)
    keep.start()

    for copy in weights:
        copy.wait()
    part = 2 * LANES if channels % (2 * LANES) == 0 else channels
    for first in range(0, channels, part):
        cols = pl.ds(first, part)
        value = jnp.dot(normed_ref[...], value_w[:, cols], preferred_element_type=jnp.float32)
        gate = jnp.dot(normed_ref[...], gate_w[:, cols], preferred_element_type=jnp.float32)
        glued = (value * jax.nn.sigmoid(gate)).astype(jnp.bfloat16)
        extended[pl.ds(HALO, rows), cols] = glued.astype(jnp.float32)
        glued_s[:, cols] = glued[rows - HALO :]

    def halo_copy():
        return remote(
            glued_s, halo_s, halo_send, halo_recv, {"sp": (me + 1) % sp_count}
        )

    @pl.when(me < sp_count - 1)
    def _():
        halo_copy().start()

    @pl.when(me == 0)
    def _():
        extended[pl.ds(0, HALO), :] = jnp.zeros((HALO, channels), jnp.float32)

    @pl.when(me > 0)
    def _():
        halo_copy().wait_recv()
        extended[pl.ds(0, HALO), :] = halo_s[...].astype(jnp.float32)

    carry_s[...] = jnp.zeros_like(carry_s)
    acc_s[...] = jnp.zeros_like(acc_s)
    sums = [jnp.zeros((rows, 1), jnp.float32)] * 2
    for first in range(0, channels, LANES):
        cols = pl.ds(first, LANES)
        conv = jnp.zeros((rows, LANES), jnp.float32)
        for tap in range(tap_count):
            weight = taps_ref[tap : tap + 1, cols].astype(jnp.float32)
            conv = conv + weight * extended[pl.ds(HALO - tap_count + 1 + tap, rows), cols]
        conv = conv.astype(jnp.bfloat16)
        conv_s[:, cols] = conv
        conv = conv.astype(jnp.float32)
        sums = [
            sums[0] + jnp.sum(conv, axis=1, keepdims=True),
            sums[1] + jnp.sum(conv * conv, axis=1, keepdims=True),
        ]
    for index in range(2):
        stat_out[8 * index : 8 * index + 8, :] = jnp.transpose(
            jnp.broadcast_to(sums[index], (rows, LANES))
        )[:8]

    def stat_copy(step):
        return remote(
            stat_out, stat_in.at[step], stat_send.at[step], stat_recv.at[step],
            {"tp": (tp_me + step) % tp_count},
        )

    for step in range(1, tp_count):
        stat_copy(step).start()
    total = stat_out[...]
    for step in range(1, tp_count):
        stat_copy(step).wait_recv()
        total = total + stat_in[step]
    all_channels = channels * tp_count
    mean = jnp.transpose(jnp.broadcast_to(total[:1], (LANES, rows))) / all_channels
    square = jnp.transpose(jnp.broadcast_to(total[8:9], (LANES, rows))) / all_channels
    inverse = lax.rsqrt(square - mean * mean + 1e-05)
    for first in range(0, channels, LANES):
        cols = pl.ds(first, LANES)
        act = (conv_s[:, cols].astype(jnp.float32) - mean) * inverse * gain_ref[:, cols]
        own_act[:, cols] = (act * jax.nn.sigmoid(act)).astype(jnp.bfloat16)

    act_spread = Spread(own_act, act_ref, *spread_sems[:4])
    act_spread.start()
    act_keep = pltpu.make_async_copy(own_act, act_spread.columns(tp_me), keep_sem)
    keep.wait()
    act_keep.start()
    act_keep.wait()

    offset = offset_ref[0, me]
    side = lax.broadcasted_iota(jnp.int32, (cell, 2 * cell), 0)
    across = lax.broadcasted_iota(jnp.int32, (cell, 2 * cell), 1)
    later = ((side > across) | (across >= cell)).astype(jnp.bfloat16)

    def one(row, key_block, col, diagonal):
        held = pl.ds(row, rows - row)
        z = (
            lax.dot_general(
                query_s[held, :], key_s[key_block, pl.ds(col, cell), :],
                (((1,), (1,)), ((), ())), preferred_element_type=jnp.float32,
            )
            * scale
            + offset
        )
        soft, own = softplus_parts(z)
        if diagonal:
            allowed = lax.broadcasted_iota(jnp.int32, z.shape, 1) <= lax.broadcasted_iota(
                jnp.int32, z.shape, 0
            )
            soft = jnp.where(allowed, soft, 0.0)
        behind = jnp.dot(soft.astype(jnp.bfloat16), later, preferred_element_type=jnp.float32)
        carry = carry_s[held, :]
        stick = jnp.exp(own - behind[:, :cell] - carry)
        if diagonal:
            stick = jnp.where(allowed, stick, 0.0)
        acc_s[held, :] += jnp.dot(
            stick.astype(jnp.bfloat16), value_s[key_block, pl.ds(col, cell), :],
            preferred_element_type=jnp.float32,
        )
        carry_s[held, :] = carry + behind[:, cell:]

    def back_copies(to, source):
        return (
            remote(
                back_out.at[to], back_in.at[source], back_send.at[to], back_recv.at[source],
                {"sp": to},
            ),
            remote(
                spent_out.at[to], spent_in.at[source], spent_send.at[to], spent_recv.at[source],
                {"sp": to},
            ),
        )

    def block(index, _):
        @pl.when(index != me)
        def _():
            step = (me - index + sp_count) % sp_count
            remote(
                packed_ref.at[index], chunks.at[index], chunk_send.at[step], chunk_recv.at[step],
                {"sp": (me + step) % sp_count},
            ).wait_recv()

        @pl.when(index == sp_count // 2)
        def _():
            act_spread.forward()

        query_s[...] = chunks[index, :rows, :width]
        key_s[index] = chunks[index, :rows, width:]
        value_s[index, :half] = chunks[index, rows:, :width]
        value_s[index, half:] = chunks[index, rows:, width:]
        acc_s[...] = jnp.zeros_like(acc_s)
        carry_s[...] = jnp.zeros_like(carry_s)
        for col in range(rows - cell, -1, -cell):
            one(col, index, col, True)

        def turn(back, _):
            for col in range(rows - cell, -1, -cell):
                one(0, index - 1 - back, col, False)
            return 0

        lax.fori_loop(0, index, turn, 0)
        done = jnp.concatenate([acc_s[:half, :], acc_s[half:, :]], axis=1).astype(jnp.bfloat16)
        spent = jnp.transpose(carry_s[...])[:8]

        @pl.when(index != me)
        def _():
            back_out[index] = done
            spent_out[index] = spent
            for copy in back_copies(index, me):
                copy.start()

        @pl.when(index == me)
        def _():
            back_in[index] = done
            spent_in[index] = spent

        return 0

    lax.fori_loop(0, sp_count, block, 0)

    for source in range(sp_count):
        @pl.when(source != me)
        def _():
            for copy in back_copies((2 * me - source + sp_count) % sp_count, source):
                copy.wait_recv()
    for part in range(2):
        own_rows[part * half : (part + 1) * half, :] = jnp.concatenate(
            [
                back_in[source][:, part * width : (part + 1) * width]
                for source in range(sp_count)
            ],
            axis=1,
        )
    last_spread = Spread(own_rows, attended_ref, *spread_sems[4:])
    last_spread.start()
    last_keep = pltpu.make_async_copy(own_rows, last_spread.columns(tp_me), keep_sem)
    last_keep.start()
    for source in range(sp_count):
        spent_ref[source : source + 1, :] = spent_in[source, :1]
    for step in range(1, sp_count):
        chunk_copy(step).wait_send()
        for copy in back_copies((me + step) % sp_count, me):
            copy.wait_send()
    for step in range(1, tp_count):
        stat_copy(step).wait_send()

    @pl.when(me < sp_count - 1)
    def _():
        halo_copy().wait_send()

    act_spread.finish()
    last_keep.wait()
    last_spread.forward()
    last_spread.finish()


def branches(packed, normed, w_value, w_gate, taps, gain, offsets, scale):
    sp_count, tall, wide = packed.shape
    width = wide // 2
    rows = normed.shape[0]
    tp_count = lax.axis_size("tp")
    channels = taps.shape[1]
    bf, f32 = jnp.bfloat16, jnp.float32
    dma = pltpu.SemaphoreType.DMA
    vmem = pl.BlockSpec(memory_space=pltpu.VMEM)
    hbm = pl.BlockSpec(memory_space=pl.ANY)
    return pl.pallas_call(
        functools.partial(branch_kernel, taps.shape[0], scale),
        in_specs=[pl.BlockSpec(memory_space=pltpu.SMEM), vmem, vmem, hbm, hbm, vmem, vmem],
        out_specs=[vmem, vmem, vmem],
        out_shape=[
            jax.ShapeDtypeStruct((rows, channels * tp_count), bf),
            jax.ShapeDtypeStruct((rows, channels * tp_count), bf),
            jax.ShapeDtypeStruct((sp_count, rows), f32),
        ],
        scratch_shapes=[
            pltpu.VMEM((sp_count, tall, wide), bf),
            pltpu.VMEM((sp_count, rows, width), bf),
            pltpu.VMEM((sp_count, rows, width), bf),
            pltpu.VMEM((rows, width), bf),
            pltpu.VMEM((rows, width), f32),
            pltpu.VMEM((rows, LANES), f32),
            pltpu.VMEM((sp_count, rows // 2, wide), bf),
            pltpu.VMEM((sp_count, rows // 2, wide), bf),
            pltpu.VMEM((sp_count, 8, rows), f32),
            pltpu.VMEM((sp_count, 8, rows), f32),
            pltpu.VMEM((rows, channels), bf),
            pltpu.VMEM(w_value.shape, bf),
            pltpu.VMEM(w_gate.shape, bf),
            pltpu.VMEM((HALO, channels), bf),
            pltpu.VMEM((HALO, channels), bf),
            pltpu.VMEM((HALO + rows, channels), f32),
            pltpu.VMEM((rows, channels), bf),
            pltpu.VMEM((rows, channels), bf),
            pltpu.VMEM((16, rows), f32),
            pltpu.VMEM((tp_count, 16, rows), f32),
            dma((2,)), dma,
            dma((sp_count,)), dma((sp_count,)), dma((sp_count,)), dma((sp_count,)),
            dma((sp_count,)), dma((sp_count,)), dma, dma, dma((tp_count,)), dma((tp_count,)),
        ] + Spread.semaphores(tp_count) + Spread.semaphores(tp_count),
        compiler_params=pltpu.CompilerParams(
            collective_id=1, has_side_effects=True, vmem_limit_bytes=48 << 20
        ),
        cost_estimate=pl.CostEstimate(
            flops=4 * sp_count * sp_count * rows * rows * width,
            bytes_accessed=8 * w_value.size,
            transcendentals=2 * sp_count * sp_count * rows * rows,
        ),
    )(offsets, packed, normed, w_value, w_gate, taps, gain)


def body(
    tokens, norm_gain, w_glu_value, w_glu_gate, w_query, w_key, w_value, score_offset, conv_taps,
    conv_gain, w_conv_out, w_attn_out, w_gate_conv, w_gate_attn,
):
    sp_count, tp_count = lax.axis_size("sp"), lax.axis_size("tp")
    rows, channels = tokens.shape[0], w_query.shape[1]
    head_count = score_offset.shape[0]
    fits = rows % LANES == 0 and channels % LANES == 0 and conv_taps.shape[0] <= HALO + 1
    if head_count != sp_count or tp_count % 2 or not fits:
        return plain_body(
            tokens, norm_gain, w_glu_value, w_glu_gate, w_query, w_key, w_value, score_offset,
            conv_taps, conv_gain, w_conv_out, w_attn_out, w_gate_conv, w_gate_attn,
        )
    width = channels // head_count
    normed = gather_normed(tokens, norm_gain)
    query, key, value = (
        jnp.dot(normed, weight, preferred_element_type=jnp.float32)
        .astype(jnp.bfloat16)
        .reshape(rows, sp_count, width)
        for weight in (w_query, w_key, w_value)
    )
    packed = jnp.concatenate(
        [
            jnp.concatenate([query, key], axis=2),
            jnp.concatenate([value[: rows // 2], value[rows // 2 :]], axis=2),
        ],
        axis=0,
    ).transpose(1, 0, 2)
    local_gain = lax.dynamic_slice_in_dim(conv_gain, lax.axis_index("tp") * channels, channels, 0)
    conv_piece, attn_piece, spent_stick = branches(
        packed, normed, w_glu_value, w_glu_gate, conv_taps, local_gain[None], score_offset[None],
        1.0 / width**0.5,
    )
    log_weight = jnp.log(-jnp.expm1(-spent_stick))
    gate_conv = jax.nn.sigmoid(jnp.dot(normed, w_gate_conv, preferred_element_type=jnp.float32))
    gate_attn = jax.nn.sigmoid(jnp.dot(normed, w_gate_attn, preferred_element_type=jnp.float32))
    conv_branch = jnp.dot(conv_piece, w_conv_out, preferred_element_type=jnp.float32)
    attn_branch = jnp.dot(attn_piece, w_attn_out, preferred_element_type=jnp.float32)
    mixed = (gate_conv * conv_branch + gate_attn * attn_branch).astype(jnp.bfloat16)
    return (mixed, log_weight)


def solution(mesh):
    in_specs = (
        P("sp", "tp"),
        P(),
        P(None, "tp"),
        P(None, "tp"),
        P(None, "tp"),
        P(None, "tp"),
        P(None, "tp"),
        P("tp"),
        P(None, "tp"),
        P(),
        P(None, "tp"),
        P(None, "tp"),
        P(None, "tp"),
        P(None, "tp"),
    )
    out_specs = (P("sp", "tp"), P("tp", "sp"))
    return jax.shard_map(body, mesh=mesh, in_specs=in_specs, out_specs=out_specs, check_vma=False)
```
